32 devices in a mesh: sp: 4 (over y, x), tp: 8 (over z, core).
Axes of the slice: x: 2, y: 2, z: 4, core: 2. Of those that a mesh axis runs over, the one named last changes fastest.
Arguments:
- stream: bfloat16 [4096, 1024], P('tp', 'sp'), may hold values from -6 to 6
- value_weight: bfloat16 [2, 2048, 4096], P(None, 'tp', 'sp'), may hold values from -0.09375 to 0.09375
- gate_weight: bfloat16 [2, 2048, 4096], P(None, 'tp', 'sp'), may hold values from -0.09375 to 0.09375
- conv_taps: bfloat16 [2, 2048, 31], P(None, 'tp'), may hold values from -16 to 16
- norm_gain: bfloat16 [2, 2048], P(None, 'tp'), may hold values from 0.099609375 to 1.8984375
- out_weight: bfloat16 [2, 4096, 2048], P(None, 'tp', 'sp'), may hold values from -4 to 4
- out_gain: bfloat16 [2, 4096], P(None, 'tp'), may hold values from 0.099609375 to 1.8984375
Outputs:
- result: bfloat16 [4096, 1024], P('tp', 'sp')
The draws below stay inside these ranges and needn't reach their ends.
All inputs are finite; a program needn't handle non-finite values.
Results may differ from the reference program's by a relative error of at most 0.015.
Values may be sent and summed in bfloat16 or wider, within the bound.
A program may use at most 64 MiB of HBM per device.

```python
import jax
import jax.numpy as jnp
from jax import lax

D = 4096
W = 2048
KERNEL = 31
LAYERS = 2
SEQ = 1024


def rising_draw(key, shape, fan, axis):
    base = jax.random.normal(key, shape, jnp.float32)
    position = lax.broadcasted_iota(jnp.float32, shape, axis) / shape[axis]
    return base * fan ** (-0.5) * jnp.exp(position * 2.302585)


def draw_conv_taps(key, part):
    return rising_draw(jax.random.fold_in(key, 11), (LAYERS, W, KERNEL), KERNEL, 1).astype(jnp.bfloat16)


def draw_out_weight(key, part):
    return rising_draw(jax.random.fold_in(key, 23), (LAYERS, D, W), W, 1).astype(jnp.bfloat16)


def levels(key, shape, cuts, least, largest):
    loudness, own = 1.0, jax.random.fold_in(key, 6)
    for dim, blocks in cuts:
        steps = jnp.exp(jax.random.uniform(jax.random.fold_in(own, dim), (blocks,), jnp.float32, least / len(cuts), largest / len(cuts)))
        loudness = loudness * jnp.repeat(steps, shape[dim] // blocks).reshape([-1 if axis == dim else 1 for axis in range(len(shape))])
    return loudness


def gaussian(own_key, extent, scale, bound, pieces=(), dtype=jnp.bfloat16):
    gain = levels(own_key, extent, pieces, -0.22, 0.18) if pieces else 1.0
    result = jax.random.normal(own_key, extent, jnp.float32) * scale * gain
    return jnp.minimum(jnp.maximum(result, -bound), bound).astype(dtype)


def setup_inputs(seed: int = 0) -> dict:
    splits = jax.random.split(jax.random.key(seed), 8)
    stream = gaussian(splits[0], (D, SEQ), 1.0, 6.0, ((0, 8), (1, 4)))
    value_weight = gaussian(splits[1], (LAYERS, W, D), D ** -0.5, 0.09375, ((1, 8), (2, 4)))
    gate_weight = gaussian(splits[2], (LAYERS, W, D), D ** -0.5, 0.09375, ((1, 8), (2, 4)))
    conv_taps = draw_conv_taps(jax.random.fold_in(splits[7], 71), 0)
    norm_gain = jnp.clip(1.0 + 0.18 * jax.random.normal(splits[4], (LAYERS, W), jnp.float32), 0.099609375, 1.8984375).astype(jnp.bfloat16)
    out_weight = draw_out_weight(jax.random.fold_in(splits[7], 71), 0)
    out_gain = jnp.clip(1.0 + 0.18 * jax.random.normal(splits[6], (LAYERS, D), jnp.float32), 0.099609375, 1.8984375).astype(jnp.bfloat16)
    return {"stream": stream, "value_weight": value_weight, "gate_weight": gate_weight, "conv_taps": conv_taps, "norm_gain": norm_gain, "out_weight": out_weight, "out_gain": out_gain}


def reference(stream, value_weight, gate_weight, conv_taps, norm_gain, out_weight, out_gain):
    hidden = stream
    reach = KERNEL // 2
    for layer_index in range(LAYERS):
        value_proj = jnp.dot(value_weight[layer_index], hidden, preferred_element_type=jnp.float32)
        gate_proj = jnp.dot(gate_weight[layer_index], hidden, preferred_element_type=jnp.float32)
        gated = (value_proj * jax.nn.sigmoid(gate_proj)).astype(jnp.bfloat16)
        padded = jnp.pad(gated.astype(jnp.float32), ((0, 0), (reach, reach)))
        kernel_taps = conv_taps[layer_index].astype(jnp.float32)
        convolved = jnp.zeros((W, SEQ), jnp.float32)
        for offset in range(KERNEL):
            convolved = convolved + kernel_taps[:, offset:offset + 1] * padded[:, offset:offset + SEQ]
        conv_wide = lax.optimization_barrier(convolved.astype(jnp.bfloat16)).astype(jnp.float32)
        average = lax.optimization_barrier(jnp.sum(conv_wide, axis=0)) / W
        variance = lax.optimization_barrier(jnp.sum(conv_wide * conv_wide, axis=0)) / W - average * average
        channel_gain = norm_gain[layer_index].astype(jnp.float32)[:, None]
        activated = jax.nn.silu((conv_wide - average) * lax.rsqrt(variance + 1e-05) * channel_gain).astype(jnp.bfloat16)
        branch = jnp.dot(out_weight[layer_index], activated, preferred_element_type=jnp.float32)
        branch_wide = lax.optimization_barrier(branch.astype(jnp.bfloat16)).astype(jnp.float32)
        square_mean = lax.optimization_barrier(jnp.sum(branch_wide * branch_wide, axis=0)) / D
        feature_gain = out_gain[layer_index].astype(jnp.float32)[:, None]
        hidden = (hidden.astype(jnp.float32) + branch_wide * lax.rsqrt(square_mean + 1e-06) * feature_gain).astype(jnp.bfloat16)
    return hidden
```

```python
import functools

import jax
import jax.numpy as jnp
from jax import lax
from jax.experimental import pallas as pl
from jax.experimental.pallas import tpu as pltpu
from jax.sharding import PartitionSpec as P

MESH = pl.DeviceIdType.MESH
F32 = jnp.float32
BF16 = jnp.bfloat16
LANES = 128
CONV_ROWS = 16


def grid_of(count):
    nx = int(count**0.5)
    while count % nx:
        nx -= 1
    return count // nx, nx


def kernel(
    n_sp, n_tp, n_layers,
    stream, value_w, gate_w, taps, norm_gain, out_w, out_gain,
    result,
    h_all, act_all, v_buf, g_buf, o_buf, gat, halo_l, halo_r, conv, acc, sums, squares,
    local_sem, send_sem, recv_sem,
):
    ny, nx = grid_of(n_sp)
    nz = n_tp // 2
    s, t = lax.axis_index("sp"), lax.axis_index("tp")
    y, x = s // nx, s % nx
    z, c = t // 2, t % 2
    features, positions = stream.shape
    channels = value_w.shape[1]
    f_cols = value_w.shape[2]
    c_cols = out_w.shape[2]
    width = channels * n_tp
    model = features * n_tp
    n_taps = taps.shape[2]
    reach = n_taps // 2
    counter = [0]
    sent = []

    def remote(src, dst, sp, tp):
        i = counter[0]
        counter[0] += 1
        return pltpu.make_async_remote_copy(
            src_ref=src, dst_ref=dst, send_sem=send_sem.at[i], recv_sem=recv_sem.at[i],
            device_id={"sp": sp, "tp": tp}, device_id_type=MESH,
        )

    def start(copy):
        copy.start()
        sent.append(copy)

    def slot_of(k, j):
        return lax.rem(y + ny - k, ny) * nx + lax.rem(x + nx - j, nx)

    def x_peer(j):
        return y * nx + lax.rem(x + j, nx)

    def y_peer(k):
        return lax.rem(y + k, ny) * nx + x

    class Gather:
        def __init__(self, src, dst, x_first):
            self.copies = {}
            for k in range(ny):
                for j in range(nx):
                    if k == 0 and j == 0:
                        continue
                    if x_first:
                        along_x = k == 0
                        origin = (0, 0) if along_x else (0, j)
                    else:
                        along_x = j > 0
                        origin = (k, 0) if along_x else (0, 0)
                    own = origin == (0, 0)
                    target = x_peer(j) if along_x else y_peer(k)
                    origin_slot = slot_of(*origin)
                    self.copies[k, j] = (
                        remote(src if own else dst(origin_slot), dst(origin_slot), target, t),
                        own, origin,
                    )
            i = local_count[0]
            local_count[0] += 1
            self.local = pltpu.make_async_copy(src, dst(s), local_sem.at[i])
            self.here = set()

        def start_own(self):
            for copy, own, _ in self.copies.values():
                if own:
                    start(copy)
            self.local.start()

        def forward(self):
            for copy, own, origin in self.copies.values():
                if not own:
                    self.arrive(*origin)
                    start(copy)

        def arrive(self, k, j):
            if (k, j) not in self.here:
                self.here.add((k, j))
                if k == 0 and j == 0:
                    self.local.wait()
                else:
                    self.copies[k, j][0].wait_recv()

    local_count = [0]

    class Spread:
        def __init__(self, buf, rows, src):
            def place(zz, cc):
                return buf.at[pl.ds(pl.multiple_of((zz * 2 + cc) * rows, rows), rows), :]

            self.along = {
                k: remote(src, place(z, c), s, lax.rem(z + k, nz) * 2 + c) for k in range(1, nz)
            }
            self.across = {0: remote(src, place(z, c), s, z * 2 + 1 - c)}
            for k in range(1, nz):
                back = lax.rem(z + nz - k, nz)
                self.across[k] = remote(place(back, c), place(back, c), s, z * 2 + 1 - c)

        def start_own(self):
            for k in self.order():
                start(self.along[k])
            start(self.across[0])

        def order(self):
            return sorted(self.along, key=lambda k: min(k, nz - k))

        def finish(self):
            for k in self.order():
                self.along[k].wait_recv()
                start(self.across[k])
            for k in self.across:
                self.across[k].wait_recv()

    def totals(buf):
        copies = []
        for k in range(1, n_tp):
            copies.append(remote(buf.at[t], buf.at[t], s, lax.rem(t + k, n_tp)))
            start(copies[-1])
        for copy in copies:
            copy.wait_recv()
        return jnp.sum(buf[...], axis=0)

    barrier = pltpu.get_barrier_semaphore()
    for k in range(1, n_sp):
        pl.semaphore_signal(
            barrier, inc=1, device_id={"sp": lax.rem(s + k, n_sp), "tp": t}, device_id_type=MESH
        )
    for k in range(1, n_tp):
        pl.semaphore_signal(
            barrier, inc=1, device_id={"sp": s, "tp": lax.rem(t + k, n_tp)}, device_id_type=MESH
        )
    pl.semaphore_wait(barrier, n_sp + n_tp - 2)

    half = features // 2
    in_proj, out_proj = [], []
    for l in range(n_layers):
        in_proj.append((
            Gather(value_w.at[l], lambda q, l=l: v_buf.at[l, q], True),
            Gather(gate_w.at[l], lambda q, l=l: g_buf.at[l, q], False),
        ))
        out_proj.append((
            Gather(out_w.at[l, pl.ds(0, half)], lambda q, l=l: o_buf.at[l, q, pl.ds(0, half)], True),
            Gather(
                out_w.at[l, pl.ds(half, half)], lambda q, l=l: o_buf.at[l, q, pl.ds(half, half)], False
            ),
        ))

    my_rows = pl.ds(pl.multiple_of(t * features, features), features)
    my_channels = pl.ds(pl.multiple_of(t * channels, channels), channels)
    stream_copy = pltpu.make_async_copy(stream, h_all.at[0, my_rows, :], local_sem.at[4 * n_layers])
    stream_copy.start()
    spread = Spread(h_all.at[0], features, stream)
    spread.start_own()
    for gather in in_proj[0]:
        gather.start_own()
    steps = [(k, j) for k in range(ny) for j in range(nx)]
    right, left = lax.rem(s + 1, n_sp), lax.rem(s + n_sp - 1, n_sp)

    for l in range(n_layers):
        spread.finish()
        if l == 0:
            stream_copy.wait()
        for gather in in_proj[l]:
            gather.forward()
        for k, j in steps:
            slot = slot_of(k, j)
            rows = pl.ds(pl.multiple_of(slot * f_cols, f_cols), f_cols)
            for half_index, (gather, buf) in enumerate(zip(in_proj[l], (v_buf, g_buf))):
                gather.arrive(k, j)
                part = jnp.dot(buf[l, slot], h_all[l, rows, :], preferred_element_type=F32)
                if (k, j) == (0, 0):
                    acc[half_index] = part
                else:
                    acc[half_index] += part
        gat[l] = (acc[0] * jax.nn.sigmoid(acc[1])).astype(BF16)

        to_right = remote(gat.at[l, :, pl.ds(positions - LANES, LANES)], halo_l.at[l], right, t)
        to_left = remote(gat.at[l, :, pl.ds(0, LANES)], halo_r.at[l], left, t)

        @pl.when(s < n_sp - 1)
        def _():
            to_right.start()

        @pl.when(s > 0)
        def _():
            to_left.start()

        for gather in out_proj[l]:
            gather.start_own()

        @pl.when(s == 0)
        def _():
            halo_l[l] = jnp.zeros_like(halo_l[l])

        @pl.when(s == n_sp - 1)
        def _():
            halo_r[l] = jnp.zeros_like(halo_r[l])

        @pl.when(s > 0)
        def _():
            to_right.wait_recv()

        @pl.when(s < n_sp - 1)
        def _():
            to_left.wait_recv()

        def conv_step(i, carry):
            rows = pl.ds(pl.multiple_of(i * CONV_ROWS, CONV_ROWS), CONV_ROWS)
            wide = jnp.concatenate(
                [halo_l[l, rows, :].astype(F32), gat[l, rows, :].astype(F32), halo_r[l, rows, :].astype(F32)],
                axis=1,
            )
            extent = wide.shape[1]
            weights = taps[l, rows, :].astype(F32)
            total = jnp.zeros((CONV_ROWS, positions), F32)
            for offset in range(n_taps):
                moved = pltpu.roll(wide, (reach - offset) % extent, 1)
                total = total + weights[:, offset : offset + 1] * moved[:, LANES : LANES + positions]
            narrow = total.astype(BF16)
            conv[rows, :] = narrow
            value = narrow.astype(F32)
            return (
                carry[0] + jnp.sum(value, axis=0, keepdims=True),
                carry[1] + jnp.sum(value * value, axis=0, keepdims=True),
            )

        zero = jnp.zeros((1, positions), F32)
        own_sum, own_square = lax.fori_loop(0, channels // CONV_ROWS, conv_step, (zero, zero))
        sums[l, t, 0:1, :] = own_sum
        sums[l, t, 1:2, :] = own_square
        channel_totals = totals(sums.at[l])
        average = channel_totals[0:1] / width
        variance = channel_totals[1:2] / width - average * average
        scaled = (conv[...].astype(F32) - average) * lax.rsqrt(variance + 1e-05) * norm_gain[l].astype(F32)
        act_all[l, my_channels, :] = (scaled / (1.0 + jnp.exp(-scaled))).astype(BF16)
        act_spread = Spread(act_all.at[l], channels, act_all.at[l, my_channels, :])
        act_spread.start_own()
        act_spread.finish()
        for gather in out_proj[l]:
            gather.forward()
        if l + 1 < n_layers:
            for gather in in_proj[l + 1]:
                gather.start_own()
        total = None
        for k, j in steps:
            slot = slot_of(k, j)
            rows = pl.ds(pl.multiple_of(slot * c_cols, c_cols), c_cols)
            for gather in out_proj[l]:
                gather.arrive(k, j)
            part = jnp.dot(o_buf[l, slot], act_all[l, rows, :], preferred_element_type=F32)
            total = part if total is None else total + part
        branch = total.astype(BF16).astype(F32)
        squares[l, t, 0:1, :] = jnp.sum(branch * branch, axis=0, keepdims=True)
        square_total = totals(squares.at[l])[0:1]
        factor = lax.rsqrt(square_total / model + 1e-06)
        fresh = h_all[l, my_rows, :].astype(F32) + branch * factor * out_gain[l].astype(F32)
        if l + 1 < n_layers:
            h_all[l + 1, my_rows, :] = fresh.astype(BF16)
            spread = Spread(h_all.at[l + 1], features, h_all.at[l + 1, my_rows, :])
            spread.start_own()
        else:
            result[...] = fresh.astype(BF16)

        @pl.when(s < n_sp - 1)
        def _():
            to_right.wait_send()

        @pl.when(s > 0)
        def _():
            to_left.wait_send()

    for copy in sent:
        copy.wait_send()


def on_device(n_sp, n_tp, stream, value_weight, gate_weight, conv_taps, norm_gain, out_weight, out_gain):
    layers, channels, f_cols = value_weight.shape
    features, positions = stream.shape
    c_cols = out_weight.shape[2]
    copies = layers * (4 * (n_sp - 1) + 2 + 4 * (n_tp - 1))
    vmem = pl.BlockSpec(memory_space=pltpu.VMEM)
    hbm = pl.BlockSpec(memory_space=pl.ANY)
    return pl.pallas_call(
        functools.partial(kernel, n_sp, n_tp, layers),
        out_shape=jax.ShapeDtypeStruct(stream.shape, BF16),
        in_specs=[hbm, hbm, hbm, vmem, vmem, hbm, vmem],
        out_specs=vmem,
        scratch_shapes=[
            pltpu.VMEM((layers, n_tp * features, positions), BF16),
            pltpu.VMEM((layers, n_tp * channels, positions), BF16),
            pltpu.VMEM((layers, n_sp, channels, f_cols), BF16),
            pltpu.VMEM((layers, n_sp, channels, f_cols), BF16),
            pltpu.VMEM((layers, n_sp, features, c_cols), BF16),
            pltpu.VMEM((layers, channels, positions), BF16),
            pltpu.VMEM((layers, channels, LANES), BF16),
            pltpu.VMEM((layers, channels, LANES), BF16),
            pltpu.VMEM((channels, positions), BF16),
            pltpu.VMEM((2, channels, positions), F32),
            pltpu.VMEM((layers, n_tp, 2, positions), F32),
            pltpu.VMEM((layers, n_tp, 1, positions), F32),
            pltpu.SemaphoreType.DMA((4 * layers + 1,)),
            pltpu.SemaphoreType.DMA((copies,)),
            pltpu.SemaphoreType.DMA((copies,)),
        ],
        compiler_params=pltpu.CompilerParams(
            collective_id=0, has_side_effects=True, vmem_limit_bytes=48 * 1024 * 1024
        ),
    )(stream, value_weight, gate_weight, conv_taps, norm_gain[:, :, None], out_weight, out_gain[:, :, None])


def solution(mesh):
    return jax.shard_map(
        functools.partial(on_device, mesh.shape["sp"], mesh.shape["tp"]),
        mesh=mesh,
        in_specs=(
            P("tp", "sp"),
            P(None, "tp", "sp"),
            P(None, "tp", "sp"),
            P(None, "tp", None),
            P(None, "tp"),
            P(None, "tp", "sp"),
            P(None, "tp"),
        ),
        out_specs=P("tp", "sp"),
        check_vma=False,
    )
```

```python
import functools

import jax
import jax.numpy as jnp
from jax import lax
from jax.experimental import pallas as pl
from jax.experimental.pallas import tpu as pltpu
from jax.sharding import PartitionSpec as P

MESH = pl.DeviceIdType.MESH
F32 = jnp.float32
BF16 = jnp.bfloat16
LANES = 128
CONV_ROWS = 16


def grid_of(count):
    nx = int(count**0.5)
    while count % nx:
        nx -= 1
    return count // nx, nx


def kernel(
    n_sp, n_tp, n_layers,
    stream, value_w, gate_w, taps, norm_gain, out_w, out_gain,
    result,
    h_all, act_all, v_buf, g_buf, o_buf, gat, halo_l, halo_r, conv, acc, sums, squares,
    local_sem, send_sem, recv_sem,
):
    ny, nx = grid_of(n_sp)
    nz = n_tp // 2
    s, t = lax.axis_index("sp"), lax.axis_index("tp")
    y, x = s // nx, s % nx
    z, c = t // 2, t % 2
    features, positions = stream.shape
    channels = value_w.shape[1]
    f_cols = value_w.shape[2]
    c_cols = out_w.shape[2]
    width = channels * n_tp
    model = features * n_tp
    n_taps = taps.shape[2]
    reach = n_taps // 2
    counter = [0]
    sent = []

    def remote(src, dst, sp, tp):
        i = counter[0]
        counter[0] += 1
        return pltpu.make_async_remote_copy(
            src_ref=src, dst_ref=dst, send_sem=send_sem.at[i], recv_sem=recv_sem.at[i],
            device_id={"sp": sp, "tp": tp}, device_id_type=MESH,
        )

    def start(copy, condition=None):
        if condition is None:
            copy.start()
        else:
            pl.when(condition)(copy.start)
        sent.append((copy, condition))

    def slot_of(k, j):
        return lax.rem(y + ny - k, ny) * nx + lax.rem(x + nx - j, nx)

    def x_peer(j):
        return y * nx + lax.rem(x + j, nx)

    def y_peer(k):
        return lax.rem(y + k, ny) * nx + x

    class Gather:
        def __init__(self, src, dst, x_first):
            self.copies = {}
            self.x_first = x_first
            for k in range(ny):
                for j in range(nx):
                    if k == 0 and j == 0:
                        continue
                    if x_first:
                        along_x = k == 0
                        origin = (0, 0) if along_x else (0, j)
                    else:
                        along_x = j > 0
                        origin = (k, 0) if along_x else (0, 0)
                    own = origin == (0, 0)
                    target = x_peer(j) if along_x else y_peer(k)
                    origin_slot = slot_of(*origin)
                    self.copies[k, j] = (
                        remote(src if own else dst(origin_slot), dst(origin_slot), target, t),
                        own, origin,
                    )
            i = local_count[0]
            local_count[0] += 1
            self.local = pltpu.make_async_copy(src, dst(s), local_sem.at[i])
            self.here = set()

        def start_own(self, first):
            for (k, j), (copy, own, _) in self.copies.items():
                if own and first == ((k == 0) == self.x_first):
                    start(copy)
            if first:
                self.local.start()

        def forward(self):
            for copy, own, origin in self.copies.values():
                if not own:
                    self.arrive(*origin)
                    start(copy)

        def arrive(self, k, j):
            if (k, j) not in self.here:
                self.here.add((k, j))
                if k == 0 and j == 0:
                    self.local.wait()
                else:
                    self.copies[k, j][0].wait_recv()

    local_count = [0]

    def start_pair(pair):
        for first in (True, False):
            for gather in pair:
                gather.start_own(first)

    def forward_pair(pair):
        for gather in pair:
            gather.forward()

    class Spread:
        def __init__(self, buf, rows, src):
            def place(zz, cc):
                row = pl.multiple_of((jnp.clip(zz, 0, nz - 1) * 2 + cc) * rows, rows)
                return buf.at[pl.ds(row, rows), :]

            self.across = remote(src, place(z, c), s, z * 2 + 1 - c)
            self.along, self.hand, self.has = {}, {}, {}
            for way in (1, -1):
                after = jnp.clip(z + way, 0, nz - 1) * 2 + c
                for d in range(1, nz):
                    carried = z - way * (d - 1)
                    origin = src if d == 1 else place(carried, c)
                    self.along[way, d] = remote(origin, place(carried, c), s, after)
                    self.has[way, d] = (z - way * d >= 0) & (z - way * d < nz)
                    seen = place(z - way * d, c)
                    self.hand[way, d] = remote(seen, seen, s, z * 2 + 1 - c)

        def send(self, way, d):
            holds = (z - way * (d - 1) >= 0) & (z - way * (d - 1) < nz)
            more = (z + way >= 0) & (z + way < nz)
            start(self.along[way, d], holds & more)

        def start_own(self):
            for way in (1, -1):
                self.send(way, 1)
            start(self.across)

        def step(self, d):
            for way in (1, -1):
                pl.when(self.has[way, d])(self.along[way, d].wait_recv)
                if d + 1 < nz:
                    self.send(way, d + 1)
                start(self.hand[way, d], self.has[way, d])

        def finish(self):
            self.across.wait_recv()
            for (way, d), hand in self.hand.items():
                pl.when(self.has[way, d])(hand.wait_recv)

    def totals(buf):
        copies = []
        for k in range(1, n_tp):
            copies.append(remote(buf.at[t], buf.at[t], s, lax.rem(t + k, n_tp)))
            start(copies[-1])
        for copy in copies:
            copy.wait_recv()
        return jnp.sum(buf[...], axis=0)

    barrier = pltpu.get_barrier_semaphore()
    for k in range(1, n_sp):
        pl.semaphore_signal(
            barrier, inc=1, device_id={"sp": lax.rem(s + k, n_sp), "tp": t}, device_id_type=MESH
        )
    for k in range(1, n_tp):
        pl.semaphore_signal(
            barrier, inc=1, device_id={"sp": s, "tp": lax.rem(t + k, n_tp)}, device_id_type=MESH
        )
    pl.semaphore_wait(barrier, n_sp + n_tp - 2)

    half = features // 2
    in_proj, out_proj = [], []
    for l in range(n_layers):
        in_proj.append((
            Gather(value_w.at[l], lambda q, l=l: v_buf.at[l, q], True),
            Gather(gate_w.at[l], lambda q, l=l: g_buf.at[l, q], False),
        ))
        out_proj.append((
            Gather(out_w.at[l, pl.ds(0, half)], lambda q, l=l: o_buf.at[l, q, pl.ds(0, half)], True),
            Gather(
                out_w.at[l, pl.ds(half, half)], lambda q, l=l: o_buf.at[l, q, pl.ds(half, half)], False
            ),
        ))

    my_rows = pl.ds(pl.multiple_of(t * features, features), features)
    my_channels = pl.ds(pl.multiple_of(t * channels, channels), channels)
    stream_copy = pltpu.make_async_copy(stream, h_all.at[0, my_rows, :], local_sem.at[4 * n_layers])
    stream_copy.start()
    spread = Spread(h_all.at[0], features, stream)
    spread.start_own()
    start_pair(in_proj[0])
    steps = [(k, j) for k in range(ny) for j in range(nx)]
    right, left = lax.rem(s + 1, n_sp), lax.rem(s + n_sp - 1, n_sp)

    for l in range(n_layers):
        for d in range(1, nz):
            if d == nz - 1 and l == 0:
                forward_pair(in_proj[0])
            spread.step(d)
        spread.finish()
        if l == 0:
            stream_copy.wait()
        for k, j in steps:
            slot = slot_of(k, j)
            rows = pl.ds(pl.multiple_of(slot * f_cols, f_cols), f_cols)
            for half_index, (gather, buf) in enumerate(zip(in_proj[l], (v_buf, g_buf))):
                gather.arrive(k, j)
                part = jnp.dot(buf[l, slot], h_all[l, rows, :], preferred_element_type=F32)
                if (k, j) == (0, 0):
                    acc[half_index] = part
                else:
                    acc[half_index] += part
        gat[l] = (acc[0] * jax.nn.sigmoid(acc[1])).astype(BF16)

        to_right = remote(gat.at[l, :, pl.ds(positions - LANES, LANES)], halo_l.at[l], right, t)
        to_left = remote(gat.at[l, :, pl.ds(0, LANES)], halo_r.at[l], left, t)

        @pl.when(s < n_sp - 1)
        def _():
            to_right.start()

        @pl.when(s > 0)
        def _():
            to_left.start()

        start_pair(out_proj[l])

        @pl.when(s == 0)
        def _():
            halo_l[l] = jnp.zeros_like(halo_l[l])

        @pl.when(s == n_sp - 1)
        def _():
            halo_r[l] = jnp.zeros_like(halo_r[l])

        @pl.when(s > 0)
        def _():
            to_right.wait_recv()

        @pl.when(s < n_sp - 1)
        def _():
            to_left.wait_recv()

        def conv_step(i, carry):
            rows = pl.ds(pl.multiple_of(i * CONV_ROWS, CONV_ROWS), CONV_ROWS)
            wide = jnp.concatenate(
                [halo_l[l, rows, :].astype(F32), gat[l, rows, :].astype(F32), halo_r[l, rows, :].astype(F32)],
                axis=1,
            )
            extent = wide.shape[1]
            weights = taps[l, rows, :].astype(F32)
            total = jnp.zeros((CONV_ROWS, positions), F32)
            for offset in range(n_taps):
                moved = pltpu.roll(wide, (reach - offset) % extent, 1)
                total = total + weights[:, offset : offset + 1] * moved[:, LANES : LANES + positions]
            narrow = total.astype(BF16)
            conv[rows, :] = narrow
            value = narrow.astype(F32)
            return (
                carry[0] + jnp.sum(value, axis=0, keepdims=True),
                carry[1] + jnp.sum(value * value, axis=0, keepdims=True),
            )

        zero = jnp.zeros((1, positions), F32)
        own_sum, own_square = lax.fori_loop(0, channels // CONV_ROWS, conv_step, (zero, zero))
        sums[l, t, 0:1, :] = own_sum
        sums[l, t, 1:2, :] = own_square
        channel_totals = totals(sums.at[l])
        average = channel_totals[0:1] / width
        variance = channel_totals[1:2] / width - average * average
        scaled = (conv[...].astype(F32) - average) * lax.rsqrt(variance + 1e-05) * norm_gain[l].astype(F32)
        act_all[l, my_channels, :] = (scaled / (1.0 + jnp.exp(-scaled))).astype(BF16)
        act_spread = Spread(act_all.at[l], channels, act_all.at[l, my_channels, :])
        act_spread.start_own()
        forward_pair(out_proj[l])
        if l + 1 < n_layers:
            start_pair(in_proj[l + 1])
        for d in range(1, nz):
            act_spread.step(d)
        act_spread.finish()
        total = None
        for k, j in steps:
            slot = slot_of(k, j)
            rows = pl.ds(pl.multiple_of(slot * c_cols, c_cols), c_cols)
            for gather in out_proj[l]:
                gather.arrive(k, j)
            part = jnp.dot(o_buf[l, slot], act_all[l, rows, :], preferred_element_type=F32)
            total = part if total is None else total + part
        branch = total.astype(BF16).astype(F32)
        squares[l, t, 0:1, :] = jnp.sum(branch * branch, axis=0, keepdims=True)
        square_total = totals(squares.at[l])[0:1]
        factor = lax.rsqrt(square_total / model + 1e-06)
        fresh = h_all[l, my_rows, :].astype(F32) + branch * factor * out_gain[l].astype(F32)
        if l + 1 < n_layers:
            h_all[l + 1, my_rows, :] = fresh.astype(BF16)
            spread = Spread(h_all.at[l + 1], features, h_all.at[l + 1, my_rows, :])
            spread.start_own()
            forward_pair(in_proj[l + 1])
        else:
            result[...] = fresh.astype(BF16)

        @pl.when(s < n_sp - 1)
        def _():
            to_right.wait_send()

        @pl.when(s > 0)
        def _():
            to_left.wait_send()

    for copy, condition in sent:
        if condition is None:
            copy.wait_send()
        else:
            pl.when(condition)(copy.wait_send)


def on_device(n_sp, n_tp, stream, value_weight, gate_weight, conv_taps, norm_gain, out_weight, out_gain):
    layers, channels, f_cols = value_weight.shape
    features, positions = stream.shape
    c_cols = out_weight.shape[2]
    copies = layers * (4 * (n_sp - 1) + 2 + 2 * (n_tp - 1) + 2 * (4 * (n_tp // 2 - 1) + 1))
    vmem = pl.BlockSpec(memory_space=pltpu.VMEM)
    hbm = pl.BlockSpec(memory_space=pl.ANY)
    return pl.pallas_call(
        functools.partial(kernel, n_sp, n_tp, layers),
        out_shape=jax.ShapeDtypeStruct(stream.shape, BF16),
        in_specs=[hbm, hbm, hbm, vmem, vmem, hbm, vmem],
        out_specs=vmem,
        scratch_shapes=[
            pltpu.VMEM((layers, n_tp * features, positions), BF16),
            pltpu.VMEM((layers, n_tp * channels, positions), BF16),
            pltpu.VMEM((layers, n_sp, channels, f_cols), BF16),
            pltpu.VMEM((layers, n_sp, channels, f_cols), BF16),
            pltpu.VMEM((layers, n_sp, features, c_cols), BF16),
            pltpu.VMEM((layers, channels, positions), BF16),
            pltpu.VMEM((layers, channels, LANES), BF16),
            pltpu.VMEM((layers, channels, LANES), BF16),
            pltpu.VMEM((channels, positions), BF16),
            pltpu.VMEM((2, channels, positions), F32),
            pltpu.VMEM((layers, n_tp, 2, positions), F32),
            pltpu.VMEM((layers, n_tp, 1, positions), F32),
            pltpu.SemaphoreType.DMA((4 * layers + 1,)),
            pltpu.SemaphoreType.DMA((copies,)),
            pltpu.SemaphoreType.DMA((copies,)),
        ],
        compiler_params=pltpu.CompilerParams(
            collective_id=0, has_side_effects=True, vmem_limit_bytes=60 * 1024 * 1024
        ),
    )(stream, value_weight, gate_weight, conv_taps, norm_gain[:, :, None], out_weight, out_gain[:, :, None])


def solution(mesh):
    return jax.shard_map(
        functools.partial(on_device, mesh.shape["sp"], mesh.shape["tp"]),
        mesh=mesh,
        in_specs=(
            P("tp", "sp"),
            P(None, "tp", "sp"),
            P(None, "tp", "sp"),
            P(None, "tp", None),
            P(None, "tp"),
            P(None, "tp", "sp"),
            P(None, "tp"),
        ),
        out_specs=P("tp", "sp"),
        check_vma=False,
    )
```

```python
import functools

import jax
import jax.numpy as jnp
from jax import lax
from jax.experimental import pallas as pl
from jax.experimental.pallas import tpu as pltpu
from jax.sharding import PartitionSpec as P

MESH = pl.DeviceIdType.MESH
F32 = jnp.float32
BF16 = jnp.bfloat16
LANES = 128
CONV_ROWS = 16


def grid_of(count):
    nx = int(count**0.5)
    while count % nx:
        nx -= 1
    return count // nx, nx


def kernel(
    n_sp, n_tp, n_layers,
    stream, value_w, gate_w, taps, norm_gain, out_w, out_gain,
    result,
    h_all, conv_all, branch_all, active, v_buf, g_buf, o_buf, gat, halo_l, halo_r, acc, sums, squares,
    norm_rows, out_rows, norm_cols, out_cols,
    local_sem, send_sem, recv_sem,
):
    ny, nx = grid_of(n_sp)
    nz = n_tp // 2
    s, t = lax.axis_index("sp"), lax.axis_index("tp")
    y, x = s // nx, s % nx
    z, c = t // 2, t % 2
    features, positions = stream.shape
    channels = value_w.shape[1]
    f_cols = value_w.shape[2]
    c_cols = out_w.shape[2]
    width = channels * n_tp
    model = features * n_tp
    n_taps = taps.shape[2]
    reach = n_taps // 2
    counter = [0]
    sent = []

    def remote(src, dst, sp, tp):
        i = counter[0]
        counter[0] += 1
        return pltpu.make_async_remote_copy(
            src_ref=src, dst_ref=dst, send_sem=send_sem.at[i], recv_sem=recv_sem.at[i],
            device_id={"sp": sp, "tp": tp}, device_id_type=MESH,
        )

    def start(copy, condition=None):
        if condition is None:
            copy.start()
        else:
            pl.when(condition)(copy.start)
        sent.append((copy, condition))

    def slot_of(k, j):
        return lax.rem(y + ny - k, ny) * nx + lax.rem(x + nx - j, nx)

    def x_peer(j):
        return y * nx + lax.rem(x + j, nx)

    def y_peer(k):
        return lax.rem(y + k, ny) * nx + x

    class Gather:
        def __init__(self, src, dst, x_first):
            self.copies = {}
            self.x_first = x_first
            for k in range(ny):
                for j in range(nx):
                    if k == 0 and j == 0:
                        continue
                    if x_first:
                        along_x = k == 0
                        origin = (0, 0) if along_x else (0, j)
                    else:
                        along_x = j > 0
                        origin = (k, 0) if along_x else (0, 0)
                    own = origin == (0, 0)
                    target = x_peer(j) if along_x else y_peer(k)
                    origin_slot = slot_of(*origin)
                    self.copies[k, j] = (
                        remote(src if own else dst(origin_slot), dst(origin_slot), target, t),
                        own, origin,
                    )
            i = local_count[0]
            local_count[0] += 1
            self.local = pltpu.make_async_copy(src, dst(s), local_sem.at[i])
            self.here = set()

        def start_own(self, first):
            for (k, j), (copy, own, _) in self.copies.items():
                if own and first == ((k == 0) == self.x_first):
                    start(copy)
            if first:
                self.local.start()

        def forward(self):
            for copy, own, origin in self.copies.values():
                if not own:
                    self.arrive(*origin)
                    start(copy)

        def arrive(self, k, j):
            if (k, j) not in self.here:
                self.here.add((k, j))
                if k == 0 and j == 0:
                    self.local.wait()
                else:
                    self.copies[k, j][0].wait_recv()

    local_count = [0]

    def start_pair(pair):
        for first in (True, False):
            for gather in pair:
                gather.start_own(first)

    def forward_pair(pair):
        for gather in pair:
            gather.forward()

    class Spread:
        def __init__(self, buf, rows, src):
            def place(zz, cc):
                row = pl.multiple_of((jnp.clip(zz, 0, nz - 1) * 2 + cc) * rows, rows)
                return buf.at[pl.ds(row, rows), :]

            self.across = remote(src, place(z, c), s, z * 2 + 1 - c)
            self.along, self.hand, self.has = {}, {}, {}
            for way in (1, -1):
                after = jnp.clip(z + way, 0, nz - 1) * 2 + c
                for d in range(1, nz):
                    carried = z - way * (d - 1)
                    origin = src if d == 1 else place(carried, c)
                    self.along[way, d] = remote(origin, place(carried, c), s, after)
                    self.has[way, d] = (z - way * d >= 0) & (z - way * d < nz)
                    seen = place(z - way * d, c)
                    self.hand[way, d] = remote(seen, seen, s, z * 2 + 1 - c)

        def send(self, way, d):
            holds = (z - way * (d - 1) >= 0) & (z - way * (d - 1) < nz)
            more = (z + way >= 0) & (z + way < nz)
            start(self.along[way, d], holds & more)

        def start_own(self):
            for way in (1, -1):
                self.send(way, 1)
            start(self.across)

        def step(self, d):
            for way in (1, -1):
                pl.when(self.has[way, d])(self.along[way, d].wait_recv)
                if d + 1 < nz:
                    self.send(way, d + 1)
                start(self.hand[way, d], self.has[way, d])

        def finish(self):
            self.across.wait_recv()
            for (way, d), hand in self.hand.items():
                pl.when(self.has[way, d])(hand.wait_recv)

    def exchange(src, buf):
        copies = []
        for k in range(1, n_tp):
            copies.append(remote(src, buf.at[t], s, lax.rem(t + k, n_tp)))
            start(copies[-1])
        return copies

    def arrived(copies):
        for copy in copies:
            copy.wait_recv()

    def drain(spread, consume, between):
        consume(t)
        spread.across.wait_recv()
        consume(z * 2 + 1 - c)
        for d in range(1, nz):
            spread.step(d)
            if d == 1:
                between()
            for way in (1, -1):
                @pl.when(spread.has[way, d])
                def _():
                    consume((z - way * d) * 2 + c)
            for way in (1, -1):
                @pl.when(spread.has[way, d])
                def _():
                    spread.hand[way, d].wait_recv()
                    consume((z - way * d) * 2 + 1 - c)

    barrier = pltpu.get_barrier_semaphore()
    for k in range(1, n_sp):
        pl.semaphore_signal(
            barrier, inc=1, device_id={"sp": lax.rem(s + k, n_sp), "tp": t}, device_id_type=MESH
        )
    for k in range(1, n_tp):
        pl.semaphore_signal(
            barrier, inc=1, device_id={"sp": s, "tp": lax.rem(t + k, n_tp)}, device_id_type=MESH
        )
    pl.semaphore_wait(barrier, n_sp + n_tp - 2)

    half = features // 2
    in_proj, out_proj = [], []
    for l in range(n_layers):
        in_proj.append((
            Gather(value_w.at[l], lambda q, l=l: v_buf.at[l, q], True),
            Gather(gate_w.at[l], lambda q, l=l: g_buf.at[l, q], False),
        ))
        out_proj.append((
            Gather(out_w.at[l, pl.ds(0, half)], lambda q, l=l: o_buf.at[l, q, pl.ds(0, half)], True),
            Gather(
                out_w.at[l, pl.ds(half, half)], lambda q, l=l: o_buf.at[l, q, pl.ds(half, half)], False
            ),
        ))

    my_rows = pl.ds(pl.multiple_of(t * features, features), features)
    my_channels = pl.ds(pl.multiple_of(t * channels, channels), channels)
    stream_copy = pltpu.make_async_copy(stream, h_all.at[0, my_rows, :], local_sem.at[4 * n_layers])
    stream_copy.start()
    spread = Spread(h_all.at[0], features, stream)
    spread.start_own()
    start_pair(in_proj[0])
    norm_rows[t] = norm_gain[...]
    out_rows[t] = out_gain[...]
    gain_copies = exchange(norm_gain, norm_rows) + exchange(out_gain, out_rows)

    def to_columns(rows_ref, cols_ref, count):
        def turn(i, carry):
            rows = rows_ref[i].astype(F32)
            fill = jnp.zeros((8 - n_layers, count), F32)
            place = pl.ds(pl.multiple_of(i * count, count), count)
            cols_ref[place, :] = jnp.concatenate([rows, fill], axis=0).T
            return carry

        lax.fori_loop(0, n_tp, turn, 0)

    steps = [(k, j) for k in range(ny) for j in range(nx)]
    right, left = lax.rem(s + 1, n_sp), lax.rem(s + n_sp - 1, n_sp)

    for l in range(n_layers):
        if l == 0:
            for d in range(1, nz):
                if d == nz - 1:
                    forward_pair(in_proj[0])
                spread.step(d)
            spread.finish()
            stream_copy.wait()
            arrived(gain_copies)
            to_columns(norm_rows, norm_cols, channels)
            to_columns(out_rows, out_cols, features)
        for k, j in steps:
            slot = slot_of(k, j)
            rows = pl.ds(pl.multiple_of(slot * f_cols, f_cols), f_cols)
            for half_index, (gather, buf) in enumerate(zip(in_proj[l], (v_buf, g_buf))):
                gather.arrive(k, j)
                part = jnp.dot(buf[l, slot], h_all[l, rows, :], preferred_element_type=F32)
                if (k, j) == (0, 0):
                    acc[half_index] = part
                else:
                    acc[half_index] += part
        gat[l] = (acc[0] * jax.nn.sigmoid(acc[1])).astype(BF16)

        to_right = remote(gat.at[l, :, pl.ds(positions - LANES, LANES)], halo_l.at[l], right, t)
        to_left = remote(gat.at[l, :, pl.ds(0, LANES)], halo_r.at[l], left, t)

        @pl.when(s < n_sp - 1)
        def _():
            to_right.start()

        @pl.when(s > 0)
        def _():
            to_left.start()

        start_pair(out_proj[l])

        @pl.when(s == 0)
        def _():
            halo_l[l] = jnp.zeros_like(halo_l[l])

        @pl.when(s == n_sp - 1)
        def _():
            halo_r[l] = jnp.zeros_like(halo_r[l])

        @pl.when(s > 0)
        def _():
            to_right.wait_recv()

        @pl.when(s < n_sp - 1)
        def _():
            to_left.wait_recv()

        def conv_step(i, carry):
            rows = pl.ds(pl.multiple_of(i * CONV_ROWS, CONV_ROWS), CONV_ROWS)
            wide = jnp.concatenate(
                [halo_l[l, rows, :].astype(F32), gat[l, rows, :].astype(F32), halo_r[l, rows, :].astype(F32)],
                axis=1,
            )
            extent = wide.shape[1]
            weights = taps[l, rows, :].astype(F32)
            total = jnp.zeros((CONV_ROWS, positions), F32)
            for offset in range(n_taps):
                moved = pltpu.roll(wide, (reach - offset) % extent, 1)
                total = total + weights[:, offset : offset + 1] * moved[:, LANES : LANES + positions]
            narrow = total.astype(BF16)
            conv_all[l, pl.ds(pl.multiple_of(t * channels + i * CONV_ROWS, CONV_ROWS), CONV_ROWS), :] = narrow
            value = narrow.astype(F32)
            return (
                carry[0] + jnp.sum(value, axis=0, keepdims=True),
                carry[1] + jnp.sum(value * value, axis=0, keepdims=True),
            )

        zero = jnp.zeros((1, positions), F32)
        own_sum, own_square = lax.fori_loop(0, channels // CONV_ROWS, conv_step, (zero, zero))
        sums[l, t, 0:1, :] = own_sum
        sums[l, t, 1:2, :] = own_square
        sum_copies = exchange(sums.at[l, t], sums.at[l])
        conv_spread = Spread(conv_all.at[l], channels, conv_all.at[l, my_channels, :])
        conv_spread.start_own()
        forward_pair(out_proj[l])
        if l + 1 < n_layers:
            start_pair(in_proj[l + 1])
        arrived(sum_copies)
        channel_totals = jnp.sum(sums[l], axis=0)
        average = channel_totals[0:1] / width
        variance = channel_totals[1:2] / width - average * average
        inverse = lax.rsqrt(variance + 1e-05)

        def activate(block):
            rows = pl.ds(pl.multiple_of(block * channels, channels), channels)
            gain = norm_cols[rows, l : l + 1]
            scaled = (conv_all[l, rows, :].astype(F32) - average) * inverse * gain
            active[rows, :] = (scaled / (1.0 + jnp.exp(-scaled))).astype(BF16)

        drain(conv_spread, activate, lambda: None)
        total = None
        for k, j in steps:
            slot = slot_of(k, j)
            rows = pl.ds(pl.multiple_of(slot * c_cols, c_cols), c_cols)
            for gather in out_proj[l]:
                gather.arrive(k, j)
            part = jnp.dot(o_buf[l, slot], active[rows, :], preferred_element_type=F32)
            total = part if total is None else total + part
        narrow_branch = total.astype(BF16)
        branch = narrow_branch.astype(F32)
        squares[l, t, 0:1, :] = jnp.sum(branch * branch, axis=0, keepdims=True)
        square_copies = exchange(squares.at[l, t], squares.at[l])
        last = l + 1 == n_layers
        if not last:
            branch_all[l, my_rows, :] = narrow_branch
            spread = Spread(branch_all.at[l], features, branch_all.at[l, my_rows, :])
            spread.start_own()
        arrived(square_copies)
        factor = lax.rsqrt(jnp.sum(squares[l], axis=0) / model + 1e-06)
        if last:
            gain = out_cols[my_rows, l : l + 1]
            fresh = h_all[l, my_rows, :].astype(F32) + branch * factor * gain
            result[...] = fresh.astype(BF16)
        else:

            def renew(block):
                rows = pl.ds(pl.multiple_of(block * features, features), features)
                gain = out_cols[rows, l : l + 1]
                change = branch_all[l, rows, :].astype(F32) * factor * gain
                h_all[l + 1, rows, :] = (h_all[l, rows, :].astype(F32) + change).astype(BF16)

            drain(spread, renew, lambda: forward_pair(in_proj[l + 1]))

        @pl.when(s < n_sp - 1)
        def _():
            to_right.wait_send()

        @pl.when(s > 0)
        def _():
            to_left.wait_send()

    for copy, condition in sent:
        if condition is None:
            copy.wait_send()
        else:
            pl.when(condition)(copy.wait_send)


def on_device(n_sp, n_tp, stream, value_weight, gate_weight, conv_taps, norm_gain, out_weight, out_gain):
    layers, channels, f_cols = value_weight.shape
    features, positions = stream.shape
    c_cols = out_weight.shape[2]
    copies = layers * (4 * (n_sp - 1) + 2 + 2 * (n_tp - 1) + 2 * (4 * (n_tp // 2 - 1) + 1)) + 2 * (n_tp - 1)
    vmem = pl.BlockSpec(memory_space=pltpu.VMEM)
    hbm = pl.BlockSpec(memory_space=pl.ANY)
    return pl.pallas_call(
        functools.partial(kernel, n_sp, n_tp, layers),
        out_shape=jax.ShapeDtypeStruct(stream.shape, BF16),
        in_specs=[hbm, hbm, hbm, vmem, vmem, hbm, vmem],
        out_specs=vmem,
        scratch_shapes=[
            pltpu.VMEM((layers, n_tp * features, positions), BF16),
            pltpu.VMEM((layers, n_tp * channels, positions), BF16),
            pltpu.VMEM((max(layers - 1, 1), n_tp * features, positions), BF16),
            pltpu.VMEM((n_tp * channels, positions), BF16),
            pltpu.VMEM((layers, n_sp, channels, f_cols), BF16),
            pltpu.VMEM((layers, n_sp, channels, f_cols), BF16),
            pltpu.VMEM((layers, n_sp, features, c_cols), BF16),
            pltpu.VMEM((layers, channels, positions), BF16),
            pltpu.VMEM((layers, channels, LANES), BF16),
            pltpu.VMEM((layers, channels, LANES), BF16),
            pltpu.VMEM((2, channels, positions), F32),
            pltpu.VMEM((layers, n_tp, 2, positions), F32),
            pltpu.VMEM((layers, n_tp, 1, positions), F32),
            pltpu.VMEM((n_tp, layers, channels), BF16),
            pltpu.VMEM((n_tp, layers, features), BF16),
            pltpu.VMEM((n_tp * channels, 8), F32),
            pltpu.VMEM((n_tp * features, 8), F32),
            pltpu.SemaphoreType.DMA((4 * layers + 1,)),
            pltpu.SemaphoreType.DMA((copies,)),
            pltpu.SemaphoreType.DMA((copies,)),
        ],
        compiler_params=pltpu.CompilerParams(
            collective_id=0, has_side_effects=True, vmem_limit_bytes=60 * 1024 * 1024
        ),
    )(stream, value_weight, gate_weight, conv_taps, norm_gain, out_weight, out_gain)


def solution(mesh):
    return jax.shard_map(
        functools.partial(on_device, mesh.shape["sp"], mesh.shape["tp"]),
        mesh=mesh,
        in_specs=(
            P("tp", "sp"),
            P(None, "tp", "sp"),
            P(None, "tp", "sp"),
            P(None, "tp", None),
            P(None, "tp"),
            P(None, "tp", "sp"),
            P(None, "tp"),
        ),
        out_specs=P("tp", "sp"),
        check_vma=False,
    )
```
